512 devices in a mesh: fs: 16 (over y, x), tp: 32 (over z, core).
Axes of the slice: x: 4, y: 4, z: 16, core: 2. Of those that a mesh axis runs over, the one named last changes fastest.
Arguments:
- tokens: bfloat16 [4096, 2048], P('fs', 'tp'), may hold values from -60 to 60
- norm_gain: float32 [2048], P('fs'), may hold values from 0.1 to 1.9
- gate_weight: float32 [16, 2048, 4096], P(None, 'fs', 'tp'), may hold values from -0.125 to 0.125
- up_weight: float32 [16, 2048, 4096], P(None, 'fs', 'tp'), may hold values from -0.125 to 0.125
- down_weight: float32 [16, 2048, 4096], P(None, 'fs', 'tp'), may hold values from -0.1875 to 0.1875
- route: int32 [4096, 2], P('fs'), may hold values from 0 to 15, all different within a row; in each aligned block of 256 rows (0 to 255, 256 to 511, ...) at most 64 rows name the same one
- route_weight: float32 [4096, 2], P('fs'), may hold values from 0.2 to 1
Outputs:
- mixed: bfloat16 [4096, 2048], P('fs', 'tp')
- gate_new: bfloat16 [16, 2048, 4096], P('fs', None, 'tp')
- up_new: bfloat16 [16, 2048, 4096], P('fs', None, 'tp')
- down_new: bfloat16 [16, 2048, 4096], P('fs', None, 'tp')
The draws below stay inside these ranges and needn't reach their ends.
Inputs may be any that keep to these rules, and one draw needn't show every extreme that they name: `route`: the 2 experts of a row differ. In each aligned block of 256 rows (the tokens of one index of fs) no expert is named by more than 64 rows, a bound that some block reaches.
All inputs are finite; a program needn't handle non-finite values.
Results may differ from the reference program's by a relative error of at most 0.024.
Values may be sent and summed in bfloat16 or wider, within the bound.
A program may use at most 64 MiB of HBM per device.

```python
import math
import jax
import jax.numpy as jnp
import numpy as np
from jax import lax

D = 2048
FF = 4096
TOP = 2
TOK_DEV = 256
EXPERTS = 16
CAP = 64
TOKENS = 4096
N_FS = 16
N_TP = 32


def draw_tokens(key, part):
    key_base = jax.random.fold_in(key, 11)
    values = jax.random.normal(key_base, (TOKENS, D), jnp.float32)
    column_scale = 0.6 * 3.0 ** (jnp.arange(D, dtype=jnp.float32) / D)
    values = jnp.clip(values * column_scale[None, :], -60.0, 60.0)
    return values.astype(jnp.bfloat16)


def strengthened(result, own_key, source, target, parts, factor):
    def block_of(dim):
        return (jnp.arange(result.shape[dim]) // (result.shape[dim] // parts)).reshape((-1,) + (1,) * (result.ndim - 1 - dim))

    first = jax.random.permutation(own_key, parts)[block_of(target)]
    other_side = (block_of(target) + parts // 2) % parts
    return jnp.where((block_of(source) == first) | (block_of(source) == other_side), factor * result, result)


def block_levels(rng, extent, cuts, least, top_value):
    gain = 1.0
    for dim, blocks in cuts:
        heights = jax.random.uniform(jax.random.fold_in(jax.random.fold_in(rng, 6), dim), (blocks,), jnp.float32, least / len(cuts), top_value / len(cuts))
        gain = gain * jnp.repeat(jnp.exp(heights), extent[dim] // blocks).reshape((-1,) + (1,) * (len(extent) - 1 - dim))
    return gain


def assign_block(stream_key, own, number, rows, amount, top, bound, slope):
    ranking = jax.random.permutation(stream_key, amount)
    heavy_load, ordinary = portions_of(amount, rows * top, bound, slope, True), portions_of(amount, rows * top, bound, slope, False)
    places = jnp.arange(amount)

    def named(tallies, offset_by):
        used = int((tallies > 0).sum())
        fixed = max(1, used // 4)
        moved = fixed + (places - fixed + offset_by * (used - fixed)) % max(1, amount - fixed)
        return jnp.zeros((amount,), jnp.int32).at[ranking[jnp.where(places < fixed, places, moved)]].set(jnp.asarray(tallies, jnp.int32))

    tallies = jnp.where(number % 4 == 0, named(heavy_load, number // 4), named(ordinary, number - number // 4 - 1))
    mixed = jax.random.permutation(jax.random.fold_in(own, 3), amount)
    donor, receiver = mixed[0:amount // 2 * 2:2], mixed[1:amount // 2 * 2:2]
    slack = jnp.minimum(tallies[donor] - 1, bound - tallies[receiver]) // 2
    slack = jnp.where((donor == ranking[0]) | (receiver == ranking[0]) | (tallies[receiver] == 0), 0, jnp.maximum(slack, 0))
    moved = jax.random.randint(jax.random.fold_in(own, 4), (amount // 2,), 0, 1 << 20) % (slack + 1)
    tallies = tallies.at[donor].add(-moved).at[receiver].add(moved)
    members = jnp.searchsorted(jnp.cumsum(tallies), jnp.arange(rows * top), side="right").astype(jnp.int32)
    table = members.reshape(top, rows).T
    table = table[jax.random.permutation(jax.random.fold_in(own, 1), rows)]
    offset_by = jax.random.randint(jax.random.fold_in(own, 2), (rows, 1), 0, top)
    return jnp.take_along_axis(table, (jnp.arange(top)[None, :] + offset_by) % top, axis=1)


def portions_of(amount, total, reach, skew, full):
    weights = [(1 << 20) // math.isqrt(grade ** skew) + 1 for grade in range(1, amount + 1)]
    largest = reach if full else min(reach, max(-(-total // amount), total * weights[0] // sum(weights)))
    least = 1 if total - largest >= amount - 1 else 0
    given, spare = [largest] + [least] * (amount - 1), total - largest - least * (amount - 1)
    while spare > 0:
        candidates = [i for i in range(1, amount) if given[i] < largest] or [i for i in range(1, amount) if given[i] < reach]
        pool, remaining = sum([weights[i] for i in candidates]), spare
        for i in candidates:
            more = min(reach - given[i], max(1, remaining * weights[i] // pool), spare)
            given[i] = given[i] + more
            spare = spare - more
    return np.array(given)


def noise(rng, dims, spread, bound, pieces=(), kind=jnp.bfloat16):
    factor_of = block_levels(rng, dims, pieces, -0.22, 0.18) if pieces else 1.0
    entries = jax.random.normal(rng, dims, jnp.float32) * spread * factor_of
    return jnp.minimum(jnp.maximum(entries, -bound), bound).astype(kind)


def gaussian_with(stream_key, extent, spread, most, split, heavy, kind=jnp.bfloat16):
    drawn = spread * jax.random.normal(stream_key, extent, jnp.float32)
    if split:
        drawn = drawn * block_levels(stream_key, extent, split, -0.22, 0.18)
    return jnp.clip(strengthened(drawn, jax.random.fold_in(stream_key, 3), *heavy), -most, most).astype(kind)


def setup_inputs(seed: int = 0) -> dict:
    streams_of = jax.random.split(jax.random.key(seed), 8)
    tokens = draw_tokens(jax.random.fold_in(streams_of[7], 71), 0)
    norm_gain = jnp.clip(1.0 + 0.18 * jax.random.normal(streams_of[1], (D,), jnp.float32), 0.1, 1.9)
    gate_weight = noise(streams_of[2], (EXPERTS, D, FF), D ** -0.5, 0.125, ((1, 16), (2, 32)), jnp.float32)
    up_weight = noise(streams_of[3], (EXPERTS, D, FF), D ** -0.5, 0.125, ((1, 16), (2, 32)), jnp.float32)
    down_weight = gaussian_with(streams_of[4], (EXPERTS, D, FF), FF ** -0.5, 0.1875, ((1, 16), (2, 32)), (2, 1, 32, 2.75), jnp.float32)
    route_keys = jax.random.split(jax.random.fold_in(streams_of[5], 1), TOKENS // TOK_DEV)
    route_turns = jax.random.permutation(jax.random.fold_in(streams_of[5], 3), TOKENS // TOK_DEV)
    route = jax.vmap(lambda own, number: assign_block(jax.random.fold_in(streams_of[5], 2), own, number, TOK_DEV, EXPERTS, TOP, CAP, 2))(route_keys, route_turns).reshape((TOKENS, TOP))
    route_weight = jnp.clip(jnp.exp(math.log(1.0) - 1.609438 * jax.random.uniform(streams_of[6], (TOKENS, TOP), jnp.float32) ** block_levels(streams_of[6], (TOKENS, TOP), ((0, 16),), -0.2, 0.2)), 0.2, 1.0)
    return {"tokens": tokens, "norm_gain": norm_gain, "gate_weight": gate_weight, "up_weight": up_weight, "down_weight": down_weight, "route": route, "route_weight": route_weight}


epsilon = 1e-05

def slot_table(route, block_rows, expert_count):
    pair_ids = route.reshape(-1, block_rows * route.shape[1])
    onehot = (pair_ids[:, :, None] == jnp.arange(expert_count, dtype=jnp.int32)[None, None, :]).astype(jnp.int32)
    before = jnp.cumsum(onehot, axis=1) - onehot
    return lax.optimization_barrier(jnp.sum(before * onehot, axis=2)).astype(jnp.int32).reshape(route.shape)

def reference(tokens, norm_gain, gate_weight, up_weight, down_weight, route, route_weight):
    gain_col = norm_gain.astype(jnp.float32)[None, :, None]
    gate_new = (gate_weight * gain_col).astype(jnp.bfloat16)
    up_new = (up_weight * gain_col).astype(jnp.bfloat16)
    down_new = down_weight.astype(jnp.bfloat16)
    tok_float = tokens.astype(jnp.float32)
    normed = (tok_float * lax.rsqrt(lax.optimization_barrier(jnp.mean(tok_float * tok_float, axis=1, keepdims=True)) + epsilon)).astype(jnp.bfloat16)
    slot_of = slot_table(route, TOK_DEV, EXPERTS)
    groups = jnp.broadcast_to((jnp.arange(TOKENS, dtype=jnp.int32) // TOK_DEV)[:, None], route.shape)
    token_index = jnp.broadcast_to(jnp.arange(TOKENS, dtype=jnp.int32)[:, None], route.shape)
    row_table = jnp.full((EXPERTS, N_FS, CAP), TOKENS, jnp.int32).at[route, groups, slot_of].set(token_index)
    padded = jnp.concatenate([normed, jnp.zeros((1, D), jnp.bfloat16)], axis=0)
    block_width = FF // N_TP

    def one_expert(operands):
        gate_e, up_e, down_e, rows_e = operands
        expert_rows = padded[rows_e.reshape(-1)]
        gate_acc = jnp.dot(expert_rows, gate_e, preferred_element_type=jnp.float32)
        up_acc = jnp.dot(expert_rows, up_e, preferred_element_type=jnp.float32)
        hidden = (jax.nn.silu(gate_acc) * up_acc).astype(jnp.bfloat16)

        def add_block(block, running):
            offset = jnp.asarray(block, jnp.int32) * block_width
            part_hidden = lax.dynamic_slice_in_dim(hidden, offset, block_width, 1)
            part_weight = lax.dynamic_slice_in_dim(down_e, offset, block_width, 1)
            term = lax.dot_general(part_hidden, part_weight, (((1,), (1,)), ((), ())), preferred_element_type=jnp.float32)
            return running + term.astype(jnp.bfloat16).astype(jnp.float32)
        summed = lax.fori_loop(0, N_TP, add_block, jnp.zeros((N_FS * CAP, D), jnp.float32))
        return summed.astype(jnp.bfloat16)
    outputs = lax.map(one_expert, (gate_new, up_new, down_new, row_table))
    flat = outputs.reshape(EXPERTS * N_FS * CAP, D)
    index = ((route * N_FS + groups) * CAP + slot_of).astype(jnp.int32)
    picked = flat[index].astype(jnp.float32)
    mixed = lax.optimization_barrier(jnp.sum(picked * route_weight.astype(jnp.float32)[:, :, None], axis=1)).astype(jnp.bfloat16)
    return (mixed, gate_new, up_new, down_new)
```

```python
import jax
import jax.numpy as jnp
from jax import lax
from jax.experimental import pallas as pl
from jax.experimental.pallas import tpu as pltpu
from jax.sharding import PartitionSpec as P

MESH = pl.DeviceIdType.MESH
EPS = 1e-05
F32 = jnp.float32
BF16 = jnp.bfloat16

FS = 16
NZ = 16
HALF = NZ // 2
QUARTERS = 4


def packed(y, p):
    lane = lax.broadcasted_iota(jnp.int32, (32, 128), 1)
    top = y[0:32, 128 * p : 128 * p + 128]
    bottom = y[32:64, 128 * p : 128 * p + 128]
    first = jnp.where(lane < 64, top, pltpu.roll(bottom, 64, 1))
    second = jnp.where(lane < 64, pltpu.roll(top, 64, 1), bottom)
    return first.astype(BF16), second.astype(BF16)


def unpacked(first, second):
    lane = lax.broadcasted_iota(jnp.int32, (32, 128), 1)
    a, b = first.astype(F32), second.astype(F32)
    top = jnp.where(lane < 64, a, pltpu.roll(b, 64, 1))
    bottom = jnp.where(lane < 64, pltpu.roll(a, 64, 1), b)
    return top.astype(BF16), bottom.astype(BF16)


def kernel(
    tok, route, rw, gain, gw, uw, dw,
    mixed, gate_o, up_o, down_o,
    wst, gus, dns, gu, dn, dn2, disp, arr, xg, ssq, hid, part, s_r, s_l, r_r, r_l, yv, back, ret, hits,
    load_sem, out_sem,
    ts_sem, tr_sem, gs_sem, gr_sem, ds_sem, dr_sem, bs_sem, br_sem,
    agrs, agrr, agls, aglr, pas, par, exs, exr, rrs, rrr, rls, rlr,
):
    fs = lax.axis_index("fs")
    tp = lax.axis_index("tp")
    z = tp // 2
    c = tp % 2
    partner = (fs, tp + 1 - 2 * c)
    right = (fs, ((z + 1) % NZ) * 2 + c)
    left = (fs, ((z + NZ - 1) % NZ) * 2 + c)

    def rcopy(src, dst, ss, rs, dev):
        return pltpu.make_async_remote_copy(
            src_ref=src, dst_ref=dst, send_sem=ss, recv_sem=rs, device_id=dev, device_id_type=MESH
        )

    def peer(k):
        return (fs + k) % FS

    loads = [
        pltpu.make_async_copy(w, wst.at[i], load_sem.at[i]) for i, w in enumerate((gw, uw, dw))
    ]
    for ld in loads:
        ld.start()

    barrier = pltpu.get_barrier_semaphore()

    @pl.loop(1, FS)
    def _(k):
        pl.semaphore_signal(barrier, inc=1, device_id=(peer(k), tp), device_id_type=MESH)

    for dev in (partner, right, left):
        pl.semaphore_signal(barrier, inc=1, device_id=dev, device_id_type=MESH)

    r0, r1 = route[0:1, :], route[1:2, :]
    ex = lax.broadcasted_iota(jnp.int32, (16, 256), 0)
    m0, m1 = ex == r0, ex == r1
    named = jnp.where(m0 | m1, 1.0, 0.0).astype(BF16)
    earlier = jnp.where(
        lax.broadcasted_iota(jnp.int32, (256, 256), 0) < lax.broadcasted_iota(jnp.int32, (256, 256), 1), 1.0, 0.0
    ).astype(BF16)
    before = jnp.dot(named, earlier, preferred_element_type=F32)
    t0 = r0 * 64 + jnp.sum(jnp.where(m0, before, 0.0), axis=0, keepdims=True).astype(jnp.int32)
    t1 = r1 * 64 + jnp.sum(jnp.where(m1, before, 0.0), axis=0, keepdims=True).astype(jnp.int32)
    row = lax.broadcasted_iota(jnp.int32, (1024, 256), 0)
    hits[0] = jnp.where(row == t0, 1.0, 0.0).astype(BF16)
    hits[1] = jnp.where(row == t1, 1.0, 0.0).astype(BF16)
    d = lax.dot_general(
        tok[...], hits[0] + hits[1], (((1,), (1,)), ((), ())), preferred_element_type=F32
    )
    for p in range(8):
        a, b = packed(d, p)
        disp[2 * p] = a
        disp[2 * p + 1] = b

    pl.semaphore_wait(barrier, FS - 1 + 3)

    def tok_copy(to, src):
        return rcopy(disp.at[to], arr.at[src], ts_sem.at[to], tr_sem.at[src], (to, tp))

    @pl.loop(1, FS)
    def _(k):
        tok_copy(peer(k), fs).start()

    arr[fs] = disp[fs]

    eye = lax.broadcasted_iota(jnp.int32, (128, 128), 0) == lax.broadcasted_iota(jnp.int32, (128, 128), 1)
    gcol = jnp.sum(jnp.where(eye, gain[...], 0.0), axis=1, keepdims=True)
    loads[0].wait()
    loads[1].wait()

    @pl.loop(0, FS)
    def _(e):
        gus[e, :, 0:128] = (wst[0, e] * gcol).astype(BF16)
        gus[e, :, 128:256] = (wst[1, e] * gcol).astype(BF16)

    def gu_copy(to, src):
        return rcopy(gus.at[to], gu.at[src], gs_sem.at[to], gr_sem.at[src], (to, tp))

    def dn_copy(to, src):
        return rcopy(dns.at[to], dn.at[src], ds_sem.at[to], dr_sem.at[src], (to, tp))

    @pl.loop(1, FS)
    def _(k):
        gu_copy(peer(k), fs).start()

    gu[fs] = gus[fs]
    loads[2].wait()

    @pl.loop(0, FS)
    def _(e):
        dns[e] = wst[2, e].astype(BF16)

    @pl.loop(1, FS)
    def _(k):
        dn_copy(peer(k), fs).start()

    dn[fs] = dns[fs]

    @pl.loop(1, FS)
    def _(k):
        tok_copy(fs, peer(k)).wait_recv()

    for p in range(8):
        top, bottom = unpacked(arr[2 * p], arr[2 * p + 1])
        xg[tp, 0:32, 128 * p : 128 * p + 128] = top
        xg[tp, 32:64, 128 * p : 128 * p + 128] = bottom

    def ag(block, s, q, ss, rs, dev):
        piece = xg.at[block, pl.ds(16 * q, 16)]
        return rcopy(piece, piece, ss.at[s, q], rs.at[s, q], dev)

    def ag_r(s, q):
        return ag(((z + NZ - s) % NZ) * 2 + c, s, q, agrs, agrr, right)

    def ag_l(s, q):
        return ag(((z + s) % NZ) * 2 + c, s, q, agls, aglr, left)

    def ag_rw(s, q):
        return ag(((z + NZ - 1 - s) % NZ) * 2 + c, s, q, agrs, agrr, right)

    def ag_lw(s, q):
        return ag(((z + 1 + s) % NZ) * 2 + c, s, q, agls, aglr, left)

    def shared(block, n):
        return rcopy(xg.at[block], xg.at[block], pas.at[n], par.at[n], partner)

    for q in range(QUARTERS):
        ag_r(0, q).start()
        ag_l(0, q).start()
    shared(tp, 0).start()

    def squares(block):
        v = xg[block].astype(F32)
        v = v * v
        t = v[0:8]
        for i in range(1, 8):
            t = t + v[8 * i : 8 * i + 8]
        return t

    ssq[...] = squares(tp)

    def ag_step(s, last):
        for q in range(QUARTERS):
            ag_rw(s, q).wait_recv()
            if not last or q < 2:
                ag_r(s + 1, q).start()
            ag_lw(s, q).wait_recv()
            if not last or q >= 2:
                ag_l(s + 1, q).start()
        br = ((z + NZ - 1 - s) % NZ) * 2 + c
        bl = ((z + 1 + s) % NZ) * 2 + c
        shared(br, 1 + 2 * s).start()
        shared(bl, 2 + 2 * s).start()
        ssq[...] += squares(br) + squares(bl)

    @pl.loop(0, HALF - 2)
    def _(s):
        ag_step(s, False)

    ag_step(HALF - 2, True)
    for q in range(2):
        ag_rw(HALF - 1, q).wait_recv()
        ag_lw(HALF - 1, q + 2).wait_recv()
    far = ((z + HALF) % NZ) * 2 + c
    shared(far, NZ - 1).start()
    ssq[...] += squares(far)

    @pl.loop(1, FS)
    def _(k):
        gu_copy(fs, peer(k)).wait_recv()

    @pl.loop(1, FS)
    def _(k):
        dn_copy(fs, peer(k)).wait_recv()

    outs = [
        pltpu.make_async_copy(gu.at[:, :, 0:128], gate_o, out_sem.at[0]),
        pltpu.make_async_copy(gu.at[:, :, 128:256], up_o, out_sem.at[1]),
        pltpu.make_async_copy(dn, down_o, out_sem.at[2]),
    ]
    for o in outs:
        o.start()
    own_half = pl.multiple_of(c * 64, 64)
    other_half = pl.multiple_of(64 - c * 64, 64)
    dn_swap = rcopy(
        dn.at[:, pl.ds(other_half, 64), :], dn2.at[:, :, 128:256], exs.at[0], exr.at[0], partner
    )
    dn_swap.start()
    dn2[:, :, 0:128] = dn[:, pl.ds(own_half, 64), :]

    other = 1 - 2 * c

    @pl.loop(0, NZ)
    def _(n):
        shared(tp + other, n).wait_recv()

    @pl.loop(0, NZ)
    def _(n):
        ssq[...] += squares(2 * n + 1 - c)

    total = jnp.sum(ssq[...], axis=0, keepdims=True)
    scale = lax.rsqrt(total / 2048.0 + EPS)
    acc = lax.dot_general(
        gu[...].reshape(2048, 256),
        xg[...].reshape(2048, 1024),
        (((0,), (0,)), ((), ())),
        preferred_element_type=F32,
    )
    g = acc[0:128] * scale
    u = acc[128:256] * scale
    hid[0:128] = (g / (1.0 + jnp.exp(-g)) * u).astype(BF16)
    hid_swap = rcopy(hid.at[0:128], hid.at[128:256], exs.at[1], exr.at[1], partner)
    hid_swap.start()
    dn_swap.wait_recv()
    hid_swap.wait_recv()

    def rs_r(s, q):
        rows = pl.ds(16 * q, 16)
        return rcopy(s_r.at[s, rows], r_r.at[s, rows], rrs.at[s, q], rrr.at[s, q], right)

    def rs_l(s, q):
        rows = pl.ds(16 * q, 16)
        return rcopy(s_l.at[s, rows], r_l.at[s, rows], rls.at[s, q], rlr.at[s, q], left)

    fa = jnp.dot(dn2[(z + HALF) % NZ], hid[...], preferred_element_type=F32).astype(BF16)
    s_r[0, 0:32] = fa[0:32]
    s_l[0, 32:64] = fa[32:64]
    for q in range(2):
        rs_r(0, q).start()
        rs_l(0, q + 2).start()
    part[...] = jnp.dot(
        dn2[...].reshape(1024, 256), hid[...], preferred_element_type=F32
    ).reshape(16, 64, 1024)

    def rs_step(s, first):
        dr = (z + HALF - s) % NZ
        dl = (z + HALF + s) % NZ
        for q in range(QUARTERS):
            rows = pl.ds(16 * q, 16)
            v = part[dr, rows]
            if not first or q < 2:
                rs_r(s - 1, q).wait_recv()
                v = v + r_r[s - 1, rows].astype(F32)
            s_r[s, rows] = v.astype(BF16)
            rs_r(s, q).start()
            v = part[dl, rows]
            if not first or q >= 2:
                rs_l(s - 1, q).wait_recv()
                v = v + r_l[s - 1, rows].astype(F32)
            s_l[s, rows] = v.astype(BF16)
            rs_l(s, q).start()

    rs_step(1, True)

    @pl.loop(2, HALF)
    def _(s):
        rs_step(s, False)

    for q in range(QUARTERS):
        rows = pl.ds(16 * q, 16)
        rs_r(HALF - 1, q).wait_recv()
        rs_l(HALF - 1, q).wait_recv()
        yv[rows] = (
            part[z, rows] + r_r[HALF - 1, rows].astype(F32) + r_l[HALF - 1, rows].astype(F32)
        )

    for p in range(8):
        a, b = packed(yv[...], p)
        back[2 * p] = a
        back[2 * p + 1] = b

    def back_copy(to, src):
        return rcopy(back.at[to], ret.at[src], bs_sem.at[to], br_sem.at[src], (to, tp))

    @pl.loop(1, FS)
    def _(k):
        back_copy(peer(k), fs).start()

    ret[fs] = back[fs]

    @pl.loop(1, FS)
    def _(k):
        tok_copy(peer(k), fs).wait_send()
        gu_copy(peer(k), fs).wait_send()
        dn_copy(peer(k), fs).wait_send()

    @pl.loop(0, NZ)
    def _(n):
        shared(tp, n).wait_send()

    @pl.loop(0, HALF - 1)
    def _(s):
        for q in range(QUARTERS):
            ag_r(s, q).wait_send()
            ag_l(s, q).wait_send()
            rs_r(s + 1, q).wait_send()
            rs_l(s + 1, q).wait_send()

    for q in range(2):
        ag_r(HALF - 1, q).wait_send()
        ag_l(HALF - 1, q + 2).wait_send()
        rs_r(0, q).wait_send()
        rs_l(0, q + 2).wait_send()
    dn_swap.wait_send()
    hid_swap.wait_send()
    for o in outs:
        o.wait()

    @pl.loop(1, FS)
    def _(k):
        back_copy(fs, peer(k)).wait_recv()

    tops, bottoms = [], []
    for p in range(8):
        top, bottom = unpacked(ret[2 * p], ret[2 * p + 1])
        tops.append(top)
        bottoms.append(bottom)
    got = jnp.concatenate(
        [jnp.concatenate(tops, axis=1), jnp.concatenate(bottoms, axis=1)], axis=0
    )
    first = jnp.dot(got, hits[0], preferred_element_type=F32)
    second = jnp.dot(got, hits[1], preferred_element_type=F32)
    mixed[...] = (first * rw[0:1, :] + second * rw[1:2, :]).astype(BF16)

    @pl.loop(1, FS)
    def _(k):
        back_copy(peer(k), fs).wait_send()


def body(tokens, norm_gain, gate_weight, up_weight, down_weight, route, route_weight):
    vm = pl.BlockSpec(memory_space=pltpu.VMEM)
    anywhere = pl.BlockSpec(memory_space=pl.ANY)
    dma = pltpu.SemaphoreType.DMA
    weight = jax.ShapeDtypeStruct((16, 128, 128), BF16)
    mixed, g, u, d = pl.pallas_call(
        kernel,
        out_shape=(jax.ShapeDtypeStruct((64, 256), BF16), weight, weight, weight),
        in_specs=[vm, vm, vm, vm, anywhere, anywhere, anywhere],
        out_specs=(vm, anywhere, anywhere, anywhere),
        scratch_shapes=[
            pltpu.VMEM((3, 16, 128, 128), F32),
            pltpu.VMEM((16, 128, 256), BF16),
            pltpu.VMEM((16, 128, 128), BF16),
            pltpu.VMEM((16, 128, 256), BF16),
            pltpu.VMEM((16, 128, 128), BF16),
            pltpu.VMEM((16, 64, 256), BF16),
            pltpu.VMEM((16, 32, 128), BF16),
            pltpu.VMEM((16, 32, 128), BF16),
            pltpu.VMEM((32, 64, 1024), BF16),
            pltpu.VMEM((8, 1024), F32),
            pltpu.VMEM((256, 1024), BF16),
            pltpu.VMEM((16, 64, 1024), F32),
            pltpu.VMEM((8, 64, 1024), BF16),
            pltpu.VMEM((8, 64, 1024), BF16),
            pltpu.VMEM((8, 64, 1024), BF16),
            pltpu.VMEM((8, 64, 1024), BF16),
            pltpu.VMEM((64, 1024), F32),
            pltpu.VMEM((16, 32, 128), BF16),
            pltpu.VMEM((16, 32, 128), BF16),
            pltpu.VMEM((2, 1024, 256), BF16),
            dma((3,)),
            dma((3,)),
            dma((16,)), dma((16,)),
            dma((16,)), dma((16,)),
            dma((16,)), dma((16,)),
            dma((16,)), dma((16,)),
            dma((8, 4)), dma((8, 4)),
            dma((8, 4)), dma((8, 4)),
            dma((16,)), dma((16,)),
            dma((2,)), dma((2,)),
            dma((8, 4)), dma((8, 4)),
            dma((8, 4)), dma((8, 4)),
        ],
        compiler_params=pltpu.CompilerParams(
            collective_id=0, has_side_effects=True, vmem_limit_bytes=50 * 1024 * 1024
        ),
        name="moe",
    )(
        tokens.T,
        route.T,
        route_weight.T,
        norm_gain.reshape(1, 128),
        gate_weight,
        up_weight,
        down_weight,
    )
    out = (1, 2048, 128)
    return mixed.T, g.reshape(out), u.reshape(out), d.reshape(out)


def solution(mesh):
    in_specs = (
        P("fs", "tp"),
        P("fs"),
        P(None, "fs", "tp"),
        P(None, "fs", "tp"),
        P(None, "fs", "tp"),
        P("fs", None),
        P("fs", None),
    )
    out_specs = (P("fs", "tp"), P("fs", None, "tp"), P("fs", None, "tp"), P("fs", None, "tp"))
    return jax.shard_map(body, mesh=mesh, in_specs=in_specs, out_specs=out_specs, check_vma=False)
```
